32 devices in a mesh: fs: 16 (over z, y, x), tp: 2 (over core).
Axes of the slice: x: 2, y: 2, z: 4, core: 2. Of those that a mesh axis runs over, the one named last changes fastest.
Arguments:
- tokens: bfloat16 [6144, 2048], P('fs'), may hold values from -6 to 6
- merged: bfloat16 [6144, 2048], P('fs'), may hold values from -6 to 6
- gain_first: float32 [2048], replicated, may hold values from 0.1 to 1.9
- gate_first: bfloat16 [2048, 2816], P('fs', 'tp'), may hold values from -0.125 to 0.125
- up_first: bfloat16 [2048, 2816], P('fs', 'tp'), may hold values from -0.125 to 0.125
- down_first: bfloat16 [2816, 2048], P('tp', 'fs'), may hold values from -0.21875 to 0.21875
- gain_second: float32 [2048], replicated, may hold values from 0.1 to 1.9
- gate_second: bfloat16 [2048, 2816], P('fs', 'tp'), may hold values from -0.125 to 0.125
- up_second: bfloat16 [2048, 2816], P('fs', 'tp'), may hold values from -0.125 to 0.125
- down_second: bfloat16 [2816, 2048], P('tp', 'fs'), may hold values from -0.21875 to 0.21875
Outputs:
- result: bfloat16 [6144, 2048], P('fs')
The draws below stay inside these ranges and needn't reach their ends.
All inputs are finite; a program needn't handle non-finite values.
Results may differ from the reference program's by a relative error of at most 0.01.
Values may be sent and summed in bfloat16 or wider, within the bound.
A program may use at most 64 MiB of HBM per device.

```python
import jax
import jax.numpy as jnp
from jax import lax

D = 2048
FF = 2816
TOKENS = 6144
N_TP = 2


def level_of(key, dims, shards, least, largest):
    level = 1.0
    for axis_at, parts in shards:
        draws = jax.random.uniform(jax.random.fold_in(jax.random.fold_in(key, 6), axis_at), (parts,), jnp.float32, least / len(shards), largest / len(shards))
        level = level * jnp.repeat(jnp.exp(draws), dims[axis_at] // parts).reshape((-1,) + (1,) * (len(dims) - 1 - axis_at))
    return level


def scatter_about(rng, dims, deviation, most, split=(), held_as=jnp.bfloat16):
    result = jax.random.normal(rng, dims, jnp.float32) * deviation
    if len(split) > 0:
        result = level_of(rng, dims, split, -0.22, 0.18) * result
    return jnp.clip(result, min=-most, max=most).astype(held_as)


def setup_inputs(seed: int = 0) -> dict:
    seeds = jax.random.split(jax.random.key(seed), 11)
    tokens = scatter_about(seeds[0], (TOKENS, D), 1.0, 6.0, ((0, 16),))
    merged = scatter_about(seeds[1], (TOKENS, D), 1.0, 6.0, ((0, 16),))
    gain_first = jnp.clip(1.0 + 0.18 * jax.random.normal(seeds[2], (D,), jnp.float32), 0.1, 1.9)
    gate_first = scatter_about(seeds[3], (D, FF), D ** -0.5, 0.125, ((0, 16), (1, 2)))
    up_first = scatter_about(seeds[4], (D, FF), D ** -0.5, 0.125, ((0, 16), (1, 2)))
    down_first = scatter_about(seeds[5], (FF, D), (FF // 4) ** -0.5, 0.21875, ((0, 2), (1, 16)))
    gain_second = jnp.clip(1.0 + 0.18 * jax.random.normal(seeds[6], (D,), jnp.float32), 0.1, 1.9)
    gate_second = scatter_about(seeds[7], (D, FF), D ** -0.5, 0.125, ((0, 16), (1, 2)))
    up_second = scatter_about(seeds[8], (D, FF), D ** -0.5, 0.125, ((0, 16), (1, 2)))
    down_second = scatter_about(seeds[9], (FF, D), (FF // 4) ** -0.5, 0.21875, ((0, 2), (1, 16)))
    return {"tokens": tokens, "merged": merged, "gain_first": gain_first, "gate_first": gate_first, "up_first": up_first, "down_first": down_first, "gain_second": gain_second, "gate_second": gate_second, "up_second": up_second, "down_second": down_second}


EPS = 1e-06

def norm_rows(values, gain):
    scale = lax.rsqrt(lax.optimization_barrier(jnp.mean(values * values, axis=-1, keepdims=True)) + EPS)
    return values * scale * gain.astype(jnp.float32)

def half_step(normed, gate_weight, up_weight, down_weight):
    gate = jnp.dot(normed, gate_weight, preferred_element_type=jnp.float32)
    up = jnp.dot(normed, up_weight, preferred_element_type=jnp.float32)
    hidden = (jax.nn.silu(gate) * up).astype(jnp.bfloat16)
    width = FF // N_TP

    def add_block(index, total):
        start = (index * width).astype(jnp.int32)
        cols = lax.dynamic_slice_in_dim(hidden, start, width, 1)
        rows = lax.dynamic_slice_in_dim(down_weight, start, width, 0)
        part = jnp.dot(cols, rows, preferred_element_type=jnp.float32).astype(jnp.bfloat16)
        part = lax.optimization_barrier(part)
        return total + part.astype(jnp.float32)
    empty = jnp.zeros((normed.shape[0], down_weight.shape[1]), jnp.float32)
    return lax.fori_loop(0, N_TP, add_block, empty)

def reference(tokens, merged, gain_first, gate_first, up_first, down_first, gain_second, gate_second, up_second, down_second):
    source = tokens.astype(jnp.float32)
    normed_first = norm_rows(source, gain_first).astype(jnp.bfloat16)
    down_a = half_step(normed_first, gate_first, up_first, down_first)
    middle = source + merged.astype(jnp.float32) + 0.5 * down_a
    normed_second = norm_rows(middle, gain_second).astype(jnp.bfloat16)
    down_b = half_step(normed_second, gate_second, up_second, down_second)
    return (middle + 0.5 * down_b).astype(jnp.bfloat16)
```

```python
import functools

import jax
import jax.numpy as jnp
from jax import lax
from jax.experimental import pallas as pl
from jax.experimental.pallas import tpu as pltpu
from jax.sharding import PartitionSpec as P

EPS = 1e-06
BF16 = jnp.bfloat16
F32 = jnp.float32
PLANE = 4
RING = 4


def norm_rows(values, gain):
    scale = lax.rsqrt(jnp.mean(values * values, axis=-1, keepdims=True) + EPS)
    return values * scale * gain


def gathered_block(normed, gate, up, down):
    gate_whole = lax.all_gather(gate, "fs", axis=0, tiled=True)
    up_whole = lax.all_gather(up, "fs", axis=0, tiled=True)
    g = jnp.dot(normed, gate_whole, preferred_element_type=F32)
    u = jnp.dot(normed, up_whole, preferred_element_type=F32)
    hidden = (jax.nn.silu(g) * u).astype(BF16)
    down_whole = lax.all_gather(down, "fs", axis=1, tiled=True)
    part = jnp.dot(hidden, down_whole, preferred_element_type=F32)
    return lax.psum(part.astype(BF16), "tp").astype(F32)


def gathered_shards(tokens, merged, gain1, g1, u1, d1, gain2, g2, u2, d2):
    source = tokens.astype(F32)
    middle = source + merged.astype(F32)
    normed = norm_rows(source, gain1).astype(BF16)
    middle = middle + 0.5 * gathered_block(normed, g1, u1, d1)
    normed = norm_rows(middle, gain2).astype(BF16)
    return (middle + 0.5 * gathered_block(normed, g2, u2, d2)).astype(BF16)


def kernel(
    tokens, merged, gain1, gain2, wa, wb, wc, wd, we, wf, out,
    w, normed1, normed2, hidden, part, own, sib, comb, rsr, middle, fin,
    p1_s, p1_r, p1_l, ring_s, ring_r, fwd_s, fwd_r,
    ag_s, ag_r, rel_s, rel_r, sib_s, sib_r, rs_s, rs_r, fin_s, fin_r,
):
    shards_in = (wa, wb, wc, wd, we, wf)
    fs = lax.axis_index("fs")
    t = lax.axis_index("tp")
    z = fs // PLANE
    p = fs % PLANE
    rows, width = tokens.shape
    half = rows // 2
    q, pw = w.shape[1], width // RING
    ds = wa.shape[1]
    qh = q // 2

    def dev(zz, pp, tt):
        return {"fs": zz * PLANE + pp, "tp": tt}

    def plane_peer(r):
        return (p + r) % PLANE

    zc, zb, zo = (z + 1) % RING, (z + RING - 1) % RING, (z + 2) % RING
    cw, ccw, sibling = dev(zc, p, t), dev(zb, p, t), dev(z, p, 1 - t)

    def remote(src, dst, s, r, to):
        return pltpu.make_async_remote_copy(
            src_ref=src, dst_ref=dst, send_sem=s, recv_sem=r,
            device_id=to, device_id_type=pl.DeviceIdType.MESH,
        )

    mine = pl.ds(pl.multiple_of(t * half, 16), half)
    other = pl.ds(pl.multiple_of((1 - t) * half, 16), half)

    barrier = pltpu.get_barrier_semaphore()
    targets = [cw, ccw, sibling] + [dev(z, plane_peer(r), t) for r in (1, 2, 3)]
    for to in targets:
        pl.semaphore_signal(barrier, inc=1, device_id=to, device_id_type=pl.DeviceIdType.MESH)
    pl.semaphore_wait(barrier, len(targets))

    def p1_lanes(pp):
        return pl.ds(pl.multiple_of((z * PLANE + pp) * ds, ds), ds)

    def p1(m, r):
        peer = plane_peer(r)
        src = shards_in[m].at[pl.ds(pl.multiple_of(peer * q, 16), q), :]
        return remote(src, w.at[m, :, p1_lanes(p)], p1_s.at[m, r - 1], p1_r.at[m, r - 1], dev(z, peer, t))

    def p1_local(m):
        src = shards_in[m].at[pl.ds(pl.multiple_of(p * q, 16), q), :]
        return pltpu.make_async_copy(src, w.at[m, :, p1_lanes(p)], p1_l.at[m])

    def p1_in(m, r):
        src = w.at[m, :, p1_lanes((p + PLANE - r) % PLANE)]
        return remote(src, src, p1_s.at[m, r - 1], p1_r.at[m, r - 1], dev(z, plane_peer(r), t))

    def start_p1(m):
        for r in (1, 2, 3):
            p1(m, r).start()
        p1_local(m).start()

    def blk(m, zz, lo=0, n=None):
        return w.at[m, pl.ds(lo, q if n is None else n), pl.ds(pl.multiple_of(zz * pw, pw), pw)]

    def ring(m, k, zz):
        return remote(blk(m, zz), blk(m, zz), ring_s.at[m, k], ring_r.at[m, k], (cw, ccw)[k])

    def fwd(m, k, zz):
        return remote(blk(m, zz, k * qh, qh), blk(m, zz, k * qh, qh), fwd_s.at[m, k], fwd_r.at[m, k], (cw, ccw)[k])

    def own_ring(m):
        p1_local(m).wait()
        for r in (1, 2, 3):
            p1_in(m, r).wait_recv()
        ring(m, 0, z).start()
        ring(m, 1, z).start()

    def service(m):
        ring(m, 0, zb).wait_recv()
        fwd(m, 0, zb).start()
        ring(m, 1, zc).wait_recv()
        fwd(m, 1, zc).start()

    def arrived(m):
        fwd(m, 0, zo).wait_recv()
        fwd(m, 1, zo).wait_recv()

    def ag(f, r, slot):
        buf = (normed1, normed2)[f]
        return remote(buf.at[slot, mine, :], buf.at[r, mine, :], ag_s.at[f, r - 1], ag_r.at[f, r - 1], dev(z, plane_peer(r), t))

    def relay(f, r, which):
        buf = (normed1, normed2)[f]
        return remote(buf.at[r, which, :], buf.at[r, which, :], rel_s.at[f, r], rel_r.at[f, r], sibling)

    def ag_start(f):
        for r in (3, 1, 2):
            ag(f, r, 0).start()

    def ag_relay(f):
        for r in (1, 2, 3):
            ag(f, r, r).wait_recv()
            relay(f, r, mine).start()

    def to_sibling(f, r):
        return remote(part.at[r], sib.at[r], sib_s.at[f, r], sib_r.at[f, r], sibling)

    def rs(f, r):
        return remote(comb.at[r - 1], rsr.at[r - 1], rs_s.at[f, r - 1], rs_r.at[f, r - 1], dev(z, (p + PLANE - r) % PLANE, t))

    def make_hidden(f, slot):
        buf = (normed1, normed2)[f]

        @pl.loop(0, 2)
        def _(i):
            at = pl.ds(pl.multiple_of(i * half, 16), half)
            x = buf[slot, at, :]
            dims = (((1,), (1,)), ((), ()))
            g = lax.dot_general(x, w[3 * f], dims, preferred_element_type=F32)
            u = lax.dot_general(x, w[3 * f + 1], dims, preferred_element_type=F32)
            hidden[slot, at, :] = (g / (1.0 + jnp.exp(-g)) * u).astype(BF16)

    def make_down(f, r):
        @pl.loop(0, RING)
        def _(c):
            at = pl.ds(pl.multiple_of(c * pw, pw), pw)
            part[r, :, at] = jnp.dot(hidden[r, other, :], w[3 * f + 2, :, at], preferred_element_type=F32).astype(BF16)

        to_sibling(f, r).start()

        @pl.loop(0, RING)
        def _(c):
            at = pl.ds(pl.multiple_of(c * pw, pw), pw)
            own[r, :, at] = jnp.dot(hidden[r, mine, :], w[3 * f + 2, :, at], preferred_element_type=F32).astype(BF16)

    step = 16

    def combine(f, r):
        to_sibling(f, r).wait_recv()

        @pl.loop(0, half // step)
        def _(i):
            at = pl.ds(pl.multiple_of(i * step, step), step)
            comb[r - 1, at, :] = (own[r, at, :].astype(F32) + sib[r, at, :].astype(F32)).astype(BF16)

        rs(f, r).start()

    def all_down(f):
        order = (3, 1, 2, 0)
        for k, r in enumerate(order):
            make_down(f, r)
            if k:
                combine(f, order[k - 1])
        to_sibling(f, 0).wait_recv()

    def reduced(at):
        total = own[0, at, :].astype(F32) + sib[0, at, :].astype(F32)
        for r in (1, 2, 3):
            total = total + rsr[r - 1, at, :].astype(F32)
        return total

    start_p1(0)
    start_p1(1)
    start_p1(2)

    @pl.loop(0, rows // step)
    def _(i):
        at = pl.ds(pl.multiple_of(i * step, step), step)
        normed1[0, at, :] = norm_rows(tokens[at, :].astype(F32), gain1[...]).astype(BF16)

    ag_start(0)
    for m in (3, 4, 5):
        start_p1(m)
    own_ring(0)
    own_ring(1)
    service(0)
    own_ring(2)
    ag_relay(0)
    service(1)
    own_ring(3)
    arrived(0)
    arrived(1)
    make_hidden(0, 0)
    for r in (1, 2, 3):
        relay(0, r, other).wait_recv()
        make_hidden(0, r)
    service(2)
    own_ring(4)
    arrived(2)
    all_down(0)
    service(3)
    own_ring(5)
    service(4)
    for r in (1, 2, 3):
        rs(0, r).wait_recv()

    @pl.loop(0, half // step)
    def _(i):
        at = pl.ds(pl.multiple_of(i * step, step), step)
        full = pl.ds(pl.multiple_of(t * half + i * step, step), step)
        value = tokens[full, :].astype(F32) + merged[full, :].astype(F32) + 0.5 * reduced(at)
        middle[at, :] = value
        normed2[0, full, :] = norm_rows(value, gain2[...]).astype(BF16)

    ag_start(1)
    relay(1, 0, mine).start()
    service(5)
    arrived(3)
    arrived(4)
    relay(1, 0, other).wait_recv()
    make_hidden(1, 0)
    ag_relay(1)
    for r in (1, 2, 3):
        relay(1, r, other).wait_recv()
        make_hidden(1, r)
    for r in range(PLANE):
        to_sibling(0, r).wait_send()
    for r in (1, 2, 3):
        rs(0, r).wait_send()
    arrived(5)
    all_down(1)
    for r in (1, 2, 3):
        rs(1, r).wait_recv()

    @pl.loop(0, half // step)
    def _(i):
        at = pl.ds(pl.multiple_of(i * step, step), step)
        full = pl.ds(pl.multiple_of(t * half + i * step, step), step)
        out[full, :] = (middle[at, :] + 0.5 * reduced(at)).astype(BF16)

    last = remote(out.at[mine, :], fin, fin_s, fin_r, sibling)
    last.start()
    for m in range(6):
        for r in (1, 2, 3):
            p1(m, r).wait_send()
        for k in range(2):
            ring(m, k, z).wait_send()
            fwd(m, k, (zb, zc)[k]).wait_send()
    for f in range(2):
        for r in (1, 2, 3):
            ag(f, r, 0).wait_send()
            relay(f, r, mine).wait_send()
    relay(1, 0, mine).wait_send()
    for r in range(PLANE):
        to_sibling(1, r).wait_send()
    for r in (1, 2, 3):
        rs(1, r).wait_send()
    last.wait_recv()
    out[other, :] = fin[...]
    last.wait_send()


def plane_shards(tokens, merged, gain1, g1, u1, d1, gain2, g2, u2, d2):
    rows, width = tokens.shape
    half = rows // 2
    q = d1.shape[0] // PLANE
    vmem = pl.BlockSpec(memory_space=pltpu.VMEM)
    dma = lambda *s: pltpu.SemaphoreType.DMA(s)
    return pl.pallas_call(
        kernel,
        out_shape=jax.ShapeDtypeStruct((rows, width), BF16),
        in_specs=[vmem] * 10,
        out_specs=vmem,
        scratch_shapes=[
            pltpu.VMEM((6, q, width), BF16),
            pltpu.VMEM((PLANE, rows, width), BF16),
            pltpu.VMEM((PLANE, rows, width), BF16),
            pltpu.VMEM((PLANE, rows, q), BF16),
            pltpu.VMEM((PLANE, half, width), BF16),
            pltpu.VMEM((PLANE, half, width), BF16),
            pltpu.VMEM((PLANE, half, width), BF16),
            pltpu.VMEM((PLANE - 1, half, width), BF16),
            pltpu.VMEM((PLANE - 1, half, width), BF16),
            pltpu.VMEM((half, width), F32),
            pltpu.VMEM((half, width), BF16),
            dma(6, 3), dma(6, 3), dma(6),
            dma(6, 2), dma(6, 2), dma(6, 2), dma(6, 2),
            dma(2, 3), dma(2, 3), dma(2, 4), dma(2, 4),
            dma(2, 4), dma(2, 4), dma(2, 3), dma(2, 3),
            pltpu.SemaphoreType.DMA, pltpu.SemaphoreType.DMA,
        ],
        compiler_params=pltpu.CompilerParams(
            collective_id=0, has_side_effects=True, vmem_limit_bytes=60 * 2**20
        ),
    )(tokens, merged, gain1[None], gain2[None], g1.T, u1.T, d1, g2.T, u2.T, d2)


def shards(n_fs, n_tp, *args):
    rows, width = args[0].shape
    hid, cols = args[5].shape
    fits = n_fs == PLANE * RING and n_tp == 2 and cols % 128 == 0
    fits = fits and hid % (32 * PLANE) == 0 and rows % 32 == 0
    return plane_shards(*args) if fits else gathered_shards(*args)


def solution(mesh):
    return jax.shard_map(
        functools.partial(shards, mesh.shape["fs"], mesh.shape["tp"]),
        mesh=mesh,
        in_specs=(
            P("fs", None),
            P("fs", None),
            P(),
            P("fs", "tp"),
            P("fs", "tp"),
            P("tp", "fs"),
            P(),
            P("fs", "tp"),
            P("fs", "tp"),
            P("tp", "fs"),
        ),
        out_specs=P("fs", None),
        check_vma=False,
    )
```

```python
import functools

import jax
import jax.numpy as jnp
from jax import lax
from jax.experimental import pallas as pl
from jax.experimental.pallas import tpu as pltpu
from jax.sharding import PartitionSpec as P

EPS = 1e-06
BF16 = jnp.bfloat16
F32 = jnp.float32
PLANE = 4
RING = 4


def norm_rows(values, gain):
    scale = lax.rsqrt(jnp.mean(values * values, axis=-1, keepdims=True) + EPS)
    return values * scale * gain


def gathered_block(normed, gate, up, down):
    gate_whole = lax.all_gather(gate, "fs", axis=0, tiled=True)
    up_whole = lax.all_gather(up, "fs", axis=0, tiled=True)
    g = jnp.dot(normed, gate_whole, preferred_element_type=F32)
    u = jnp.dot(normed, up_whole, preferred_element_type=F32)
    hidden = (jax.nn.silu(g) * u).astype(BF16)
    down_whole = lax.all_gather(down, "fs", axis=1, tiled=True)
    part = jnp.dot(hidden, down_whole, preferred_element_type=F32)
    return lax.psum(part.astype(BF16), "tp").astype(F32)


def gathered_shards(tokens, merged, gain1, g1, u1, d1, gain2, g2, u2, d2):
    source = tokens.astype(F32)
    middle = source + merged.astype(F32)
    normed = norm_rows(source, gain1).astype(BF16)
    middle = middle + 0.5 * gathered_block(normed, g1, u1, d1)
    normed = norm_rows(middle, gain2).astype(BF16)
    return (middle + 0.5 * gathered_block(normed, g2, u2, d2)).astype(BF16)


def kernel(
    tokens, merged, gain1, gain2, wa, wb, wc, wd, we, wf, out,
    w, normed1, normed2, hidden, part, own, sib, comb, diag, rsr, middle, fin,
    p1_s, p1_r, p1_l, ring_s, ring_r, fwd_s, fwd_r,
    ag_s, ag_r, rel_s, rel_r, sib_s, sib_r, rs_s, rs_r, fin_s, fin_r,
):
    shards_in = (wa, wb, wc, wd, we, wf)
    fs = lax.axis_index("fs")
    t = lax.axis_index("tp")
    z = fs // PLANE
    p = fs % PLANE
    rows, width = tokens.shape
    half = rows // 2
    quarter = half // 2
    q, pw = w.shape[1], width // RING
    ds = wa.shape[1]
    qh = q // 2

    def dev(zz, pp, tt):
        return {"fs": zz * PLANE + pp, "tp": tt}

    peers = (p, p + 1 - 2 * (p % 2), (p + 2) % PLANE, PLANE - 1 - p)

    zc, zb, zo = (z + 1) % RING, (z + RING - 1) % RING, (z + 2) % RING
    cw, ccw, sibling = dev(zc, p, t), dev(zb, p, t), dev(z, p, 1 - t)
    to_peer = [dev(z, pp, t) for pp in peers]

    def remote(src, dst, s, r, to):
        return pltpu.make_async_remote_copy(
            src_ref=src, dst_ref=dst, send_sem=s, recv_sem=r,
            device_id=to, device_id_type=pl.DeviceIdType.MESH,
        )

    mine = pl.ds(pl.multiple_of(t * half, 16), half)
    other = pl.ds(pl.multiple_of((1 - t) * half, 16), half)

    barrier = pltpu.get_barrier_semaphore()
    targets = [cw, ccw, sibling] + to_peer[1:]
    for to in targets:
        pl.semaphore_signal(barrier, inc=1, device_id=to, device_id_type=pl.DeviceIdType.MESH)
    pl.semaphore_wait(barrier, len(targets))

    def p1_lanes(pp):
        return pl.ds(pl.multiple_of((z * PLANE + pp) * ds, ds), ds)

    def p1(m, r):
        src = shards_in[m].at[pl.ds(pl.multiple_of(peers[r] * q, 16), q), :]
        return remote(src, w.at[m, :, p1_lanes(p)], p1_s.at[m, r - 1], p1_r.at[m, r - 1], to_peer[r])

    def p1_local(m):
        src = shards_in[m].at[pl.ds(pl.multiple_of(p * q, 16), q), :]
        return pltpu.make_async_copy(src, w.at[m, :, p1_lanes(p)], p1_l.at[m])

    def p1_in(m, r):
        src = w.at[m, :, p1_lanes(peers[r])]
        return remote(src, src, p1_s.at[m, r - 1], p1_r.at[m, r - 1], to_peer[r])

    def start_p1(m):
        for r in (3, 1, 2):
            p1(m, r).start()
        p1_local(m).start()

    def blk(m, zz, lo=0, n=None):
        return w.at[m, pl.ds(lo, q if n is None else n), pl.ds(pl.multiple_of(zz * pw, pw), pw)]

    def ring(m, k, zz):
        return remote(blk(m, zz), blk(m, zz), ring_s.at[m, k], ring_r.at[m, k], (cw, ccw)[k])

    def fwd(m, k, zz):
        return remote(blk(m, zz, k * qh, qh), blk(m, zz, k * qh, qh), fwd_s.at[m, k], fwd_r.at[m, k], (cw, ccw)[k])

    def own_ring(m):
        p1_local(m).wait()
        for r in (1, 2, 3):
            p1_in(m, r).wait_recv()
        ring(m, 0, z).start()
        ring(m, 1, z).start()

    def service(m):
        ring(m, 0, zb).wait_recv()
        fwd(m, 0, zb).start()
        ring(m, 1, zc).wait_recv()
        fwd(m, 1, zc).start()

    def arrived(m):
        fwd(m, 0, zo).wait_recv()
        fwd(m, 1, zo).wait_recv()

    bufs = (normed1, normed2)

    def piece(tt, h):
        return pl.ds(pl.multiple_of(tt * half + h * quarter, 16), quarter)

    def ag(f, r, h):
        at = piece(t, h)
        return remote(bufs[f].at[0, at, :], bufs[f].at[r, at, :], ag_s.at[f, r - 1, h], ag_r.at[f, r - 1, h], to_peer[r])

    def ag_on(f, h):
        at = piece(t, h)
        return remote(bufs[f].at[2 - h, at, :], bufs[f].at[3, at, :], ag_s.at[f, 2, h], ag_r.at[f, 2, h], to_peer[1 + h])

    def relay(f, r, h, tt):
        at = bufs[f].at[r, piece(tt, h), :]
        return remote(at, at, rel_s.at[f, r, h], rel_r.at[f, r, h], sibling)

    def ag_near(f):
        for r, h in ((2, 0), (1, 1)):
            ag(f, r, h).wait_recv()
            ag_on(f, h).start()
            relay(f, r, h, t).start()
        for r, h in ((2, 1), (1, 0)):
            ag(f, r, h).wait_recv()
            relay(f, r, h, t).start()

    def ag_far(f):
        for h in range(2):
            ag_on(f, h).wait_recv()
            relay(f, 3, h, t).start()

    def relayed(f, r):
        for h in range(2):
            relay(f, r, h, 1 - t).wait_recv()

    lanes = [pl.ds(pl.multiple_of(zz * pw, pw), pw) for zz in (z, zb, zc, zo)]
    first, second = pl.ds(0, quarter), pl.ds(quarter, quarter)

    def to_sibling(f, c, r):
        return remote(part.at[r, :, lanes[c]], sib.at[r, :, lanes[c]], sib_s.at[f, c, r], sib_r.at[f, c, r], sibling)

    def rs(f, c, kind):
        at = lanes[c]
        src, dst, r = (
            (comb.at[2, first, at], diag.at[0, :, at], 1),
            (comb.at[2, second, at], diag.at[1, :, at], 2),
            (comb.at[0, first, at], rsr.at[0, first, at], 1),
            (comb.at[0, second, at], rsr.at[0, second, at], 1),
            (comb.at[1, second, at], rsr.at[1, second, at], 2),
            (comb.at[1, first, at], rsr.at[1, first, at], 2),
        )[kind]
        return remote(src, dst, rs_s.at[f, c, kind], rs_r.at[f, c, kind], to_peer[r])

    def make_hidden(f, slot):
        @pl.loop(0, 2)
        def _(i):
            at = pl.ds(pl.multiple_of(i * half, 16), half)
            x = bufs[f][slot, at, :]
            dims = (((1,), (1,)), ((), ()))
            g = lax.dot_general(x, w[3 * f], dims, preferred_element_type=F32)
            u = lax.dot_general(x, w[3 * f + 1], dims, preferred_element_type=F32)
            hidden[slot, at, :] = (g / (1.0 + jnp.exp(-g)) * u).astype(BF16)

    def make_down(f, c):
        at = lanes[c]

        @pl.loop(0, PLANE)
        def _(k):
            r = PLANE - 1 - k
            part[r, :, at] = jnp.dot(hidden[r, other, :], w[3 * f + 2, :, at], preferred_element_type=F32).astype(BF16)
            to_sibling(f, c, r).start()
            own[r, :, at] = jnp.dot(hidden[r, mine, :], w[3 * f + 2, :, at], preferred_element_type=F32).astype(BF16)

    step = 16

    def down(f, c):
        at = lanes[c]
        make_down(f, c)
        for r, kinds in ((3, (0, 1)), (1, (2,)), (2, (4,))):
            to_sibling(f, c, r).wait_recv()

            @pl.loop(0, half // (2 * step))
            def _(i):
                some = pl.ds(pl.multiple_of(i * 2 * step, step), 2 * step)
                comb[r - 1, some, at] = (own[r, some, at].astype(F32) + sib[r, some, at].astype(F32)).astype(BF16)

            for kind in kinds:
                rs(f, c, kind).start()
        to_sibling(f, c, 0).wait_recv()

    def finish(f, c):
        at = lanes[c]
        rs(f, c, 0).wait_recv()
        comb[1, first, at] = (comb[1, first, at].astype(F32) + diag[0, :, at].astype(F32)).astype(BF16)
        rs(f, c, 5).start()
        rs(f, c, 1).wait_recv()
        comb[0, second, at] = (comb[0, second, at].astype(F32) + diag[1, :, at].astype(F32)).astype(BF16)
        rs(f, c, 3).start()

    def all_down(f, before_last):
        down(f, 0)
        service(3 * f + 2)
        before_last()
        down(f, 1)
        finish(f, 0)
        down(f, 2)
        finish(f, 1)
        arrived(3 * f + 2)
        down(f, 3)
        finish(f, 2)
        finish(f, 3)

    def landed(f):
        for c in range(RING):
            for kind in (2, 3, 4, 5):
                rs(f, c, kind).wait_recv()

    def reduced(at):
        total = own[0, at, :].astype(F32) + sib[0, at, :].astype(F32)
        return total + rsr[0, at, :].astype(F32) + rsr[1, at, :].astype(F32)

    start_p1(0)
    start_p1(1)
    start_p1(2)

    @pl.loop(0, rows // step)
    def _(i):
        at = pl.ds(pl.multiple_of(i * step, step), step)
        normed1[0, at, :] = norm_rows(tokens[at, :].astype(F32), gain1[...]).astype(BF16)

    for r, h in ((2, 0), (1, 1), (2, 1), (1, 0)):
        ag(0, r, h).start()
    for m in (3, 4, 5):
        start_p1(m)
    own_ring(0)
    own_ring(1)
    service(0)
    own_ring(2)
    ag_near(0)
    service(1)
    own_ring(3)
    ag_far(0)
    arrived(0)
    arrived(1)
    for r in range(PLANE):
        if r:
            relayed(0, r)
        make_hidden(0, r)
    all_down(0, lambda: own_ring(4))
    service(3)
    own_ring(5)
    landed(0)
    for h in range(2):

        @pl.loop(0, quarter // step)
        def _(i):
            at = pl.ds(pl.multiple_of(h * quarter + i * step, step), step)
            full = pl.ds(pl.multiple_of(t * half + h * quarter + i * step, step), step)
            value = tokens[full, :].astype(F32) + merged[full, :].astype(F32) + 0.5 * reduced(at)
            middle[at, :] = value
            normed2[0, full, :] = norm_rows(value, gain2[...]).astype(BF16)

        for r in (2 - h, 1 + h):
            ag(1, r, h).start()
        relay(1, 0, h, t).start()

    ag_near(1)
    service(4)
    ag_far(1)
    arrived(3)
    arrived(4)
    for r in range(PLANE):
        relayed(1, r)
        make_hidden(1, r)
    for c in range(RING):
        for r in range(PLANE):
            to_sibling(0, c, r).wait_send()
        for kind in range(6):
            rs(0, c, kind).wait_send()
    all_down(1, lambda: None)
    landed(1)

    @pl.loop(0, half // step)
    def _(i):
        at = pl.ds(pl.multiple_of(i * step, step), step)
        full = pl.ds(pl.multiple_of(t * half + i * step, step), step)
        out[full, :] = (middle[at, :] + 0.5 * reduced(at)).astype(BF16)

    last = remote(out.at[mine, :], fin, fin_s, fin_r, sibling)
    last.start()
    for m in range(6):
        for r in (1, 2, 3):
            p1(m, r).wait_send()
        for k in range(2):
            ring(m, k, z).wait_send()
            fwd(m, k, (zb, zc)[k]).wait_send()
    for f in range(2):
        for h in range(2):
            for r in (1, 2):
                ag(f, r, h).wait_send()
            ag_on(f, h).wait_send()
            for r in range(1 - f, PLANE):
                relay(f, r, h, t).wait_send()
    for c in range(RING):
        for r in range(PLANE):
            to_sibling(1, c, r).wait_send()
        for kind in range(6):
            rs(1, c, kind).wait_send()
    last.wait_recv()
    out[other, :] = fin[...]
    last.wait_send()


def plane_shards(tokens, merged, gain1, g1, u1, d1, gain2, g2, u2, d2):
    rows, width = tokens.shape
    half = rows // 2
    q = d1.shape[0] // PLANE
    vmem = pl.BlockSpec(memory_space=pltpu.VMEM)
    dma = lambda *s: pltpu.SemaphoreType.DMA(s)
    return pl.pallas_call(
        kernel,
        out_shape=jax.ShapeDtypeStruct((rows, width), BF16),
        in_specs=[vmem] * 10,
        out_specs=vmem,
        scratch_shapes=[
            pltpu.VMEM((6, q, width), BF16),
            pltpu.VMEM((PLANE, rows, width), BF16),
            pltpu.VMEM((PLANE, rows, width), BF16),
            pltpu.VMEM((PLANE, rows, q), BF16),
            pltpu.VMEM((PLANE, half, width), BF16),
            pltpu.VMEM((PLANE, half, width), BF16),
            pltpu.VMEM((PLANE, half, width), BF16),
            pltpu.VMEM((PLANE - 1, half, width), BF16),
            pltpu.VMEM((2, half // 2, width), BF16),
            pltpu.VMEM((2, half, width), BF16),
            pltpu.VMEM((half, width), F32),
            pltpu.VMEM((half, width), BF16),
            dma(6, 3), dma(6, 3), dma(6),
            dma(6, 2), dma(6, 2), dma(6, 2), dma(6, 2),
            dma(2, 3, 2), dma(2, 3, 2), dma(2, 4, 2), dma(2, 4, 2),
            dma(2, RING, 4), dma(2, RING, 4), dma(2, RING, 6), dma(2, RING, 6),
            pltpu.SemaphoreType.DMA, pltpu.SemaphoreType.DMA,
        ],
        compiler_params=pltpu.CompilerParams(
            collective_id=0, has_side_effects=True, vmem_limit_bytes=60 * 2**20
        ),
    )(tokens, merged, gain1[None], gain2[None], g1.T, u1.T, d1, g2.T, u2.T, d2)


def shards(n_fs, n_tp, *args):
    rows, width = args[0].shape
    hid, cols = args[5].shape
    fits = n_fs == PLANE * RING and n_tp == 2 and cols % 128 == 0
    fits = fits and hid % (32 * PLANE) == 0 and rows % 64 == 0
    return plane_shards(*args) if fits else gathered_shards(*args)


def solution(mesh):
    return jax.shard_map(
        functools.partial(shards, mesh.shape["fs"], mesh.shape["tp"]),
        mesh=mesh,
        in_specs=(
            P("fs", None),
            P("fs", None),
            P(),
            P("fs", "tp"),
            P("fs", "tp"),
            P("tp", "fs"),
            P(),
            P("fs", "tp"),
            P("fs", "tp"),
            P("tp", "fs"),
        ),
        out_specs=P("fs", None),
        check_vma=False,
    )
```
